32 devices in a mesh: ra: 4 (over z), cb: 4 (over y, x), dp: 2 (over core).
Axes of the slice: x: 2, y: 2, z: 4, core: 2. Of those that a mesh axis runs over, the one named last changes fastest.
Arguments:
- tokens: bfloat16 [3072, 4096], P('dp', 'ra'), may hold values from -20 to 20
- pre_gain: float32 [4096], P('ra'), may hold values from 0.1 to 1.9
- up_weight: bfloat16 [4096, 16384], P('ra', 'cb'), may hold values from -0.09375 to 0.09375
- up_bias: float32 [16384], P('cb'), may hold values from -4 to 4
- down_weight: bfloat16 [16384, 4096], P('cb', 'ra'), may hold values from -0.046875 to 0.046875
- post_gain: float32 [4096], P('ra'), may hold values from 0.1 to 1.9
Outputs:
- stream_out: bfloat16 [3072, 4096], P('dp', 'ra')
The draws below stay inside these ranges and needn't reach their ends.
All inputs are finite; a program needn't handle non-finite values.
Results may differ from the reference program's by a relative error of at most 0.0051.
Values may be sent and summed in bfloat16 or wider, within the bound.
A program may use at most 128 MiB of HBM per device.

```python
import jax
import jax.numpy as jnp
from jax import lax

D = 4096
FF = 16384
TOKENS = 3072


def draw_tokens(key, part):
    first, second, third = jax.random.split(key, 3)
    column = jnp.exp(jax.random.uniform(second, (D // 16,), jnp.float32, -1.2, 1.2))
    column = jnp.repeat(column, 16)
    values = jax.random.normal(first, (TOKENS, D), jnp.float32) * column
    return jnp.clip(values, -20.0, 20.0).astype(jnp.bfloat16)


def block_scale(rng, shape, cuts, low, largest):
    gain = 1.0
    for axis_at, shards_of in cuts:
        draws = jax.random.uniform(jax.random.fold_in(jax.random.fold_in(rng, 6), axis_at), (shards_of,), jnp.float32, low / len(cuts), largest / len(cuts))
        gain = gain * jnp.repeat(jnp.exp(draws), shape[axis_at] // shards_of).reshape((-1,) + (1,) * (len(shape) - 1 - axis_at))
    return gain


def bell_draw(own_key, shape, deviation, limit, shards=(), held_as=jnp.bfloat16):
    drawn = jax.random.normal(own_key, shape, jnp.float32) * deviation
    if len(shards) > 0:
        drawn = block_scale(own_key, shape, shards, -0.22, 0.18) * drawn
    return jnp.clip(drawn, min=-limit, max=limit).astype(held_as)


def setup_inputs(seed: int = 0) -> dict:
    seeds = jax.random.split(jax.random.key(seed), 7)
    return {
        "tokens": draw_tokens(jax.random.fold_in(seeds[6], 71), 0),
        "pre_gain": jnp.clip(1.0 + 0.18 * jax.random.normal(seeds[1], (D,), jnp.float32), 0.1, 1.9),
        "up_weight": bell_draw(seeds[2], (D, FF), D ** -0.5, 0.09375, ((0, 4), (1, 4))),
        "up_bias": bell_draw(seeds[3], (FF,), 1.0, 4.0, ((0, 4),), jnp.float32),
        "down_weight": bell_draw(seeds[4], (FF, D), FF ** -0.5, 0.046875, ((0, 4), (1, 4))),
        "post_gain": jnp.clip(1.0 + 0.18 * jax.random.normal(seeds[5], (D,), jnp.float32), 0.1, 1.9),
    }


epsilon = 1e-06
residual_weight = 0.5

def reference(tokens, pre_gain, up_weight, up_bias, down_weight, post_gain):
    stream = tokens.astype(jnp.float32)
    energy = lax.optimization_barrier(jnp.sum(stream * stream, axis=1))
    inverse = lax.rsqrt(energy / D + epsilon)
    scaled = (stream * pre_gain).astype(jnp.bfloat16)
    pre = jnp.dot(scaled, up_weight, preferred_element_type=jnp.float32) * inverse[:, None] + up_bias
    hidden = jnp.square(jax.nn.relu(pre)).astype(jnp.bfloat16)
    branch = jnp.dot(hidden, down_weight, preferred_element_type=jnp.float32)
    branch_energy = lax.optimization_barrier(jnp.sum(branch * branch, axis=1))
    normed = branch * lax.rsqrt(branch_energy / D + epsilon)[:, None] * post_gain
    return (residual_weight * stream + normed).astype(jnp.bfloat16)
```

```python
import jax
import jax.numpy as jnp
from jax import lax
from jax.sharding import PartitionSpec as P

epsilon = 1e-06
residual_weight = 0.5


def ring_order(count):
    if count & (count - 1):
        return list(range(count))
    return [i ^ (i >> 1) for i in range(count)]


def hop(value, axis, order, step):
    count = len(order)
    pairs = [(order[p], order[(p + step) % count]) for p in range(count)]
    return lax.ppermute(value, axis, pairs)


def axis_total(value, axis, count):
    parts = [hop(value, axis, list(range(count)), s) for s in range(1, count)]
    return value + sum(parts)


def reduce_ring(term, axis, order, place, step):
    count = len(order)
    total = term((place - step) % count) if count > 1 else term(place)
    for s in range(1, count):
        arrived = hop(total.astype(jnp.bfloat16), axis, order, step)
        total = term((place - step * (s + 1)) % count) + arrived.astype(jnp.float32)
    return total


def make_body(ra, cb, dp):
    ra_order, cb_order, dp_order = list(range(ra)), ring_order(cb), list(range(dp))
    cb_place = [cb_order.index(i) for i in range(cb)]

    def body(tokens, pre_gain, up_weight, up_bias, down_weight, post_gain):
        rows, depth = tokens.shape
        width = depth * ra
        units = up_weight.shape[1] // ra
        few = rows // cb
        me, core = lax.axis_index("ra"), lax.axis_index("dp")
        place = jnp.array(cb_place, jnp.int32)[lax.axis_index("cb")]
        bias = lax.dynamic_slice_in_dim(up_bias, me * units, units, 0)

        def spread(value):
            columns = value.shape[1] // 2
            sides = []
            for side in range(2):
                step = 1 - 2 * side
                block = value[:, side * columns:(side + 1) * columns]
                whole = jnp.zeros((rows, columns), value.dtype)
                whole = lax.dynamic_update_slice_in_dim(whole, block, place * few, 0)
                for s in range(1, cb):
                    block = hop(block, "cb", cb_order, step)
                    whole = lax.dynamic_update_slice_in_dim(whole, block, ((place - step * s) % cb) * few, 0)
                sides.append(whole)
            return sides

        def share(piece):
            part = piece.shape[0]
            whole = jnp.zeros((part * dp, piece.shape[1]), piece.dtype)
            whole = lax.dynamic_update_slice_in_dim(whole, piece, core * part, 0)
            for s in range(1, dp):
                other = hop(piece, "dp", dp_order, s)
                whole = lax.dynamic_update_slice_in_dim(whole, other, ((core - s) % dp) * part, 0)
            return whole

        def dot(a, b):
            return jnp.dot(a, b, preferred_element_type=jnp.float32)

        stream = tokens.astype(jnp.float32)
        scaled = (stream * pre_gain).astype(jnp.bfloat16)
        inverse = lax.rsqrt(axis_total(jnp.sum(stream * stream, axis=1), "ra", ra) / width + epsilon)

        quarter = lax.dynamic_slice_in_dim(scaled, place * few, few, 0)
        gathered = [hop(quarter, "ra", ra_order, s) for s in range(1, ra)]
        part = depth // dp
        up_pieces = []
        for s in range(1, ra):
            piece = lax.dynamic_slice(up_weight, (core * part, ((me + s) % ra) * units), (part, units))
            up_pieces.append(hop(piece, "ra", ra_order, s))
        pre = dot(scaled, lax.dynamic_slice_in_dim(up_weight, me * units, units, 1))
        half = depth // 2
        for value, piece in zip(gathered, up_pieces):
            first, second = spread(value)
            weight = share(piece)
            pre = pre + dot(first, weight[:half]) + dot(second, weight[half:])
        hidden = jnp.square(jax.nn.relu(pre * inverse[:, None] + bias)).astype(jnp.bfloat16)

        part = units // dp
        down_blocks = []
        for s in range(1, ra):
            piece = lax.dynamic_slice_in_dim(down_weight, ((me + s) % ra) * units + core * part, part, 0)
            piece, _ = lax.optimization_barrier((piece, up_pieces[-1]))
            down_blocks.append(share(hop(piece, "ra", ra_order, s)))

        def group_sum(weight):
            sides = []
            for side in range(2):
                columns = weight.shape[1] // 2
                branch = dot(hidden, weight[:, side * columns:(side + 1) * columns])
                term = lambda block: lax.dynamic_slice_in_dim(branch, block * few, few, 0)
                sides.append(reduce_ring(term, "cb", cb_order, place, 1 - 2 * side))
            return jnp.concatenate(sides, axis=1)

        branch = group_sum(lax.dynamic_slice_in_dim(down_weight, me * units, units, 0))
        arrived = []
        for s in range(1, ra):
            arrived.append(hop(group_sum(down_blocks[s - 1]).astype(jnp.bfloat16), "ra", ra_order, -s))
        for value in arrived:
            branch = branch + value.astype(jnp.float32)

        energy = axis_total(jnp.sum(branch * branch, axis=1), "ra", ra)
        normed = branch * lax.rsqrt(energy / width + epsilon)[:, None] * post_gain
        kept = lax.dynamic_slice_in_dim(tokens, place * few, few, 0).astype(jnp.float32)
        return jnp.concatenate(spread((residual_weight * kept + normed).astype(jnp.bfloat16)), axis=1)

    return body


def solution(mesh):
    in_specs = (P("dp", "ra"), P("ra"), P("ra", "cb"), P("cb"), P("cb", "ra"), P("ra"))
    out_specs = P("dp", "ra")
    body = make_body(mesh.shape["ra"], mesh.shape["cb"], mesh.shape["dp"])
    return jax.shard_map(body, mesh=mesh, in_specs=in_specs, out_specs=out_specs, check_vma=False)
```
